512 devices in a mesh: grp: 2 (over y), fs: 32 (over z), tp: 8 (over x, core).
Axes of the slice: x: 4, y: 2, z: 32, core: 2. Of those that a mesh axis runs over, the one named last changes fastest.
The devices are a block of a 4x8x32 slice.
Arguments:
- prompt: bfloat16 [4096, 2048], P(('grp', 'tp')), parts along dimension 0, may hold values from -6 to 6
- gain_first: float32 [2048], P('fs'), may hold values from 0.1 to 1.9
- gate_first: float32 [2048, 4096], P('fs', 'tp'), may hold values from -0.125 to 0.125
- up_first: float32 [2048, 4096], P('fs', 'tp'), may hold values from -0.125 to 0.125
- down_first: float32 [4096, 2048], P('fs', 'tp'), may hold values from -0.09375 to 0.09375
- gain_second: float32 [2048], P('fs'), may hold values from 0.1 to 1.9
- gate_second: float32 [2048, 4096], P('fs', 'tp'), may hold values from -0.125 to 0.125
- up_second: float32 [2048, 4096], P('fs', 'tp'), may hold values from -0.125 to 0.125
- down_second: float32 [4096, 2048], P('fs', 'tp'), may hold values from -0.09375 to 0.09375
Outputs:
- result: bfloat16 [4096, 2048], P(('grp', 'tp')), parts along dimension 0
- served_gate_first: bfloat16 [4096, 4096], P('grp', 'fs'), parts along dimension 0
- served_up_first: bfloat16 [4096, 4096], P('grp', 'fs'), parts along dimension 0
- served_down_first: bfloat16 [4096, 4096], P('fs', 'grp'), parts along dimension 1
- served_gate_second: bfloat16 [4096, 4096], P('grp', 'fs'), parts along dimension 0
- served_up_second: bfloat16 [4096, 4096], P('grp', 'fs'), parts along dimension 0
- served_down_second: bfloat16 [4096, 4096], P('fs', 'grp'), parts along dimension 1
The draws below stay inside these ranges and needn't reach their ends.
There are 2 independent parts, one for each index of `grp`. The reference program is written for one: setup_inputs(seed, part) draws one part's arguments, and reference() takes and returns one part's arrays. A program takes and returns all parts, laid end to end along the dimension named above; an argument that names none is the same for every part. Nothing has to cross between parts.
All inputs are finite; a program needn't handle non-finite values.
Results may differ from the reference program's by a relative error of at most 0.0053.
Values may be sent and summed in bfloat16 or wider, within the bound.
A program may use at most 64 MiB of HBM per device.

```python
import jax
import jax.numpy as jnp
from jax import lax

D = 2048
FF = 4096
TOKENS = 2048


def block_scale(rng, extent, shards, low, top_value):
    factor_of, own = 1.0, jax.random.fold_in(rng, 6)
    for position, blocks in shards:
        draws = jnp.exp(jax.random.uniform(jax.random.fold_in(own, position), (blocks,), jnp.float32, low / len(shards), top_value / len(shards)))
        factor_of = factor_of * jnp.repeat(draws, extent[position] // blocks).reshape([-1 if axis == position else 1 for axis in range(len(extent))])
    return factor_of


def gaussian(stream_key, dims, deviation, most, pieces=(), dtype=jnp.bfloat16):
    entries = deviation * jax.random.normal(stream_key, dims, jnp.float32)
    if pieces:
        entries = entries * block_scale(stream_key, dims, pieces, -0.22, 0.18)
    return jnp.clip(entries, -most, most).astype(dtype)


def setup_inputs(seed: int = 0, part: int = 0) -> dict:
    splits = jax.random.split(jax.random.key(seed), 10)
    own_keys = jax.random.split(jax.random.fold_in(splits[9], part), 10)
    return {
        "prompt": gaussian(own_keys[0], (TOKENS, D), 1.0, 6.0, ((0, 8),)),
        "gain_first": jnp.clip(1.0 + 0.18 * jax.random.normal(splits[1], (D,), jnp.float32), 0.1, 1.9),
        "gate_first": gaussian(splits[2], (D, FF), D ** -0.5, 0.125, ((0, 32), (1, 8)), jnp.float32),
        "up_first": gaussian(splits[3], (D, FF), D ** -0.5, 0.125, ((0, 32), (1, 8)), jnp.float32),
        "down_first": gaussian(splits[4], (FF, D), FF ** -0.5, 0.09375, ((0, 32), (1, 8)), jnp.float32),
        "gain_second": jnp.clip(1.0 + 0.18 * jax.random.normal(splits[5], (D,), jnp.float32), 0.1, 1.9),
        "gate_second": gaussian(splits[6], (D, FF), D ** -0.5, 0.125, ((0, 32), (1, 8)), jnp.float32),
        "up_second": gaussian(splits[7], (D, FF), D ** -0.5, 0.125, ((0, 32), (1, 8)), jnp.float32),
        "down_second": gaussian(splits[8], (FF, D), FF ** -0.5, 0.09375, ((0, 32), (1, 8)), jnp.float32),
    }


EPS = 1e-06

def fold(gain, weight):
    return (gain[:, None] * weight).astype(jnp.bfloat16)

def normed_of(stream):
    return (stream * lax.rsqrt(lax.optimization_barrier(jnp.mean(stream * stream, axis=-1, keepdims=True)) + EPS)).astype(jnp.bfloat16)

def block(stream, w_gate, w_up, w_down):
    normed = normed_of(stream)
    gate = jnp.dot(normed, w_gate, preferred_element_type=jnp.float32)
    up_val = jnp.dot(normed, w_up, preferred_element_type=jnp.float32)
    hidden = (jax.nn.silu(gate) * up_val).astype(jnp.bfloat16)
    return stream + 0.5 * jnp.dot(hidden, w_down, preferred_element_type=jnp.float32)

def reference(prompt, gain_first, gate_first, up_first, down_first, gain_second, gate_second, up_second, down_second):
    g_one = fold(gain_first, gate_first)
    u_one = fold(gain_first, up_first)
    d_one = down_first.astype(jnp.bfloat16)
    g_two = fold(gain_second, gate_second)
    u_two = fold(gain_second, up_second)
    d_two = down_second.astype(jnp.bfloat16)
    stream = prompt.astype(jnp.float32)
    stream = block(stream, g_one, u_one, d_one)
    stream = block(stream, g_two, u_two, d_two)
    return (stream.astype(jnp.bfloat16), g_one, u_one, d_one, g_two, u_two, d_two)
```

```python
import functools

import jax
import jax.numpy as jnp
from jax import lax
from jax.experimental import pallas as pl
from jax.experimental.pallas import tpu as pltpu
from jax.sharding import PartitionSpec as P

EPS = 1e-06
CORES = 2
MESH = pl.DeviceIdType.MESH


def rcopy(src, dst, send_sem, recv_sem, **where):
    return pltpu.make_async_remote_copy(
        src_ref=src, dst_ref=dst, send_sem=send_sem, recv_sem=recv_sem,
        device_id=where, device_id_type=MESH,
    )


def wait_bytes(ref, sem):
    pltpu.make_async_copy(ref, ref, sem).wait()


def kernel(
    Z, T,
    prompt, folded, downs,
    result, sg1, su1, sd1, sg2, su2, sd2,
    A, B, C, DN, NX, part, RL, RR, SL, SR, N,
    a_send, a_recv, b_send, b_recv, c_send, c_recv, p_recv, d_send, d_recv,
    rl_send, rl_recv, rr_send, rr_recv, gr_send, gr_recv, gl_send, gl_recv,
    loc, out_sem,
):
    z = lax.axis_index("fs")
    t = lax.axis_index("tp")
    X = T // CORES
    x, c = t // CORES, t % CORES
    H = Z // 2
    mats, rows, width = folded.shape
    rq = rows // X
    hid = DN.shape[1]
    zper = width // hid
    dcol = downs.shape[2]
    tok, D = NX.shape
    own = tok // Z
    half = D // 2
    right, left = lax.rem(z + 1, Z), lax.rem(z + Z - 1, Z)
    partner = t + 1 - 2 * c

    barrier = pltpu.get_barrier_semaphore()

    @pl.loop(1, Z)
    def _(k):
        pl.semaphore_signal(barrier, inc=1, device_id={"fs": lax.rem(z + k, Z)}, device_id_type=MESH)

    @pl.loop(1, T)
    def _(k):
        pl.semaphore_signal(barrier, inc=1, device_id={"tp": lax.rem(t + k, T)}, device_id_type=MESH)

    pl.semaphore_wait(barrier, Z + T - 2)

    def slice_of(layer, tt):
        return folded.at[2 * layer + tt // X, pl.ds(pl.multiple_of(lax.rem(tt, X) * rq, rq), rq), :]

    for layer in range(2):
        @pl.loop(1, T)
        def _(k):
            tt = lax.rem(t + k, T)
            rcopy(slice_of(layer, tt), A.at[layer, t], a_send.at[layer], a_recv.at[layer], tp=tt).start()

        pltpu.make_async_copy(slice_of(layer, t), A.at[layer, t], a_recv.at[layer]).start()

    for layer in range(2):
        mine = DN.at[layer, :, pl.ds(pl.multiple_of(t * dcol, dcol), dcol)]

        @pl.loop(1, T)
        def _(k):
            tt = lax.rem(t + k, T)
            rcopy(downs.at[layer], mine, d_send.at[layer], d_recv.at[layer], tp=tt).start()

        pltpu.make_async_copy(downs.at[layer], mine, d_recv.at[layer]).start()

    @pl.loop(0, tok // 16)
    def _(i):
        r = pl.ds(pl.multiple_of(i * 16, 16), 16)
        v = prompt[r, :].astype(jnp.float32)
        NX[r, :] = (v * lax.rsqrt(jnp.mean(v * v, axis=-1, keepdims=True) + EPS)).astype(jnp.bfloat16)

    pair = prompt[pl.ds(pl.multiple_of((z // 2) * 16, 16), 16), :].astype(jnp.float32)
    stream = jnp.where(lax.rem(z, 2) == 0, pair[:own], pair[own:])
    stream = jnp.concatenate([stream[:, :half], stream[:, half:]], axis=0)

    def block_for(layer, zz):
        return A.at[layer, zz // zper, :, pl.ds(pl.multiple_of(lax.rem(zz, zper) * hid, hid), hid)]

    def spread(layer, k):
        @pl.when(k < H)
        def _():
            zz = lax.rem(z + Z - k, Z)
            rcopy(block_for(layer, zz), B.at[layer, z], b_send.at[layer], b_recv.at[layer], fs=zz).start()

        zz = lax.rem(z + k, Z)
        rcopy(block_for(layer, zz), B.at[layer, z], b_send.at[layer], b_recv.at[layer], fs=zz).start()

    def spread_own(layer):
        pltpu.make_async_copy(block_for(layer, z), B.at[layer, z], b_recv.at[layer]).start()

    def rows_of(layer, tt):
        return C.at[2 * layer + tt // X, :, lax.rem(tt, X)]

    def gather_start(layer):
        wait_bytes(B.at[layer], b_recv.at[layer])
        for k in range(1, X):
            tt = lax.rem(t + CORES * k, T)
            rcopy(B.at[layer], rows_of(layer, t), c_send.at[layer], c_recv.at[layer, k - 1], tp=tt).start()
        rcopy(B.at[layer], rows_of(layer, t), c_send.at[layer], p_recv.at[layer], tp=partner).start()
        pltpu.make_async_copy(B.at[layer], rows_of(layer, t), loc.at[layer]).start()

    def gather_pass(layer):
        for k in (1, 3, 2) if X == 4 else range(1, X):
            tt = lax.rem(t + T - CORES * k, T)
            pltpu.make_async_copy(rows_of(layer, tt), rows_of(layer, tt), c_recv.at[layer, k - 1]).wait()
            rcopy(rows_of(layer, tt), rows_of(layer, tt), c_send.at[layer], p_recv.at[layer], tp=partner).start()

    def gather_end(layer):
        wait_bytes(C.at[2 * layer], p_recv.at[layer])
        pltpu.make_async_copy(B.at[layer], B.at[layer], loc.at[layer]).wait()
        for m, out in enumerate(((sg1, su1), (sg2, su2))[layer]):
            pltpu.make_async_copy(C.at[2 * layer + m], out, out_sem.at[2 * layer + m]).start()

    def partial_sums(layer):
        normed = NX[...]
        gate = jnp.dot(normed, C[2 * layer].reshape(D, hid), preferred_element_type=jnp.float32)
        up = jnp.dot(normed, C[2 * layer + 1].reshape(D, hid), preferred_element_type=jnp.float32)
        hidden = (gate / (1.0 + jnp.exp(-gate)) * up).astype(jnp.bfloat16)
        wait_bytes(DN.at[layer], d_recv.at[layer])
        pltpu.make_async_copy(DN.at[layer], (sd1, sd2)[layer], out_sem.at[4 + layer]).start()
        for h in range(2):
            got = jnp.dot(hidden, DN[layer, :, h * half:(h + 1) * half], preferred_element_type=jnp.float32)
            part[:, h * own:(h + 1) * own, :] = got.reshape(Z, own, half)

    def reduce_scatter(layer, beside):
        def step(s, first):
            dl = lax.rem(z + Z - H + s, Z)
            to_left = part[dl]
            if not first:
                pltpu.make_async_copy(RL.at[layer, s - 1], RL.at[layer, s - 1], rl_recv.at[layer, s - 1]).wait()
                to_left = to_left + RL[layer, s - 1].astype(jnp.float32)
            SL[layer, s] = to_left.astype(jnp.bfloat16)
            rcopy(SL.at[layer, s], RL.at[layer, s], rl_send.at[layer], rl_recv.at[layer, s], fs=left).start()

            def go_right():
                dr = lax.rem(z + H - 1 - s, Z)
                to_right = part[dr]
                if not first:
                    pltpu.make_async_copy(RR.at[layer, s - 1], RR.at[layer, s - 1], rr_recv.at[layer, s - 1]).wait()
                    to_right = to_right + RR[layer, s - 1].astype(jnp.float32)
                SR[layer, s] = to_right.astype(jnp.bfloat16)
                rcopy(SR.at[layer, s], RR.at[layer, s], rr_send.at[layer], rr_recv.at[layer, s], fs=right).start()

            if first:
                go_right()
            else:
                pl.when(s < H - 1)(go_right)
            beside(s)

        step(0, True)

        @pl.loop(1, H)
        def _(s):
            step(s, False)

        pltpu.make_async_copy(RR.at[layer, H - 2], RR.at[layer, H - 2], rr_recv.at[layer, H - 2]).wait()
        pltpu.make_async_copy(RL.at[layer, H - 1], RL.at[layer, H - 1], rl_recv.at[layer, H - 1]).wait()
        return part[z] + RR[layer, H - 2].astype(jnp.float32) + RL[layer, H - 1].astype(jnp.float32)

    def all_gather(layer, s0, s1):
        def step(s, first):
            ro = lax.rem(z + Z - s, Z)
            if not first:
                pltpu.make_async_copy(N.at[layer, ro], N.at[layer, ro], gr_recv.at[layer, s - 1]).wait()
            rcopy(N.at[layer, ro], N.at[layer, ro], gr_send.at[layer], gr_recv.at[layer, s], fs=right).start()

            def go_left():
                lo = lax.rem(z + s, Z)
                if not first:
                    pltpu.make_async_copy(N.at[layer, lo], N.at[layer, lo], gl_recv.at[layer, s - 1]).wait()
                rcopy(N.at[layer, lo], N.at[layer, lo], gl_send.at[layer], gl_recv.at[layer, s], fs=left).start()

            if first:
                go_left()
            else:
                pl.when(s < H - 1)(go_left)

        if s0 == 0:
            step(0, True)

        @pl.loop(max(s0, 1), s1)
        def _(s):
            step(s, False)

        if s1 == H:
            lo, ro = lax.rem(z + H - 1, Z), lax.rem(z + Z - H, Z)
            pltpu.make_async_copy(N.at[layer, lo], N.at[layer, lo], gl_recv.at[layer, H - 2]).wait()
            pltpu.make_async_copy(N.at[layer, ro], N.at[layer, ro], gr_recv.at[layer, H - 1]).wait()

    def in_rows(layer, out):
        @pl.loop(0, Z // 2)
        def _(i):
            a = N[layer, 2 * i].astype(jnp.float32)
            b = N[layer, 2 * i + 1].astype(jnp.float32)
            r = pl.ds(pl.multiple_of(i * 16, 16), 16)
            out[r, :half] = jnp.concatenate([a[:own], b[:own]], axis=0).astype(jnp.bfloat16)
            out[r, half:] = jnp.concatenate([a[own:], b[own:]], axis=0).astype(jnp.bfloat16)

    wait_bytes(A.at[0], a_recv.at[0])
    spread_own(0)

    @pl.loop(0, H)
    def _(i):
        spread(0, H - i)

    gather_start(0)
    gather_pass(0)
    gather_end(0)
    partial_sums(0)

    wait_bytes(A.at[1], a_recv.at[1])
    spread_own(1)
    total = reduce_scatter(0, lambda s: spread(1, s + 1))
    stream = stream + 0.5 * total
    mean = jnp.sum(stream * stream, axis=-1, keepdims=True)
    mean = (mean[:own] + mean[own:]) / D
    mean = jnp.concatenate([mean, mean], axis=0)
    N[0, z] = (stream * lax.rsqrt(mean + EPS)).astype(jnp.bfloat16)
    gather_start(1)
    mid = (H * 5) // 8
    all_gather(0, 0, mid)
    gather_pass(1)
    all_gather(0, mid, H)
    in_rows(0, NX)
    gather_end(1)
    partial_sums(1)
    total = reduce_scatter(1, lambda s: None)
    stream = stream + 0.5 * total
    N[1, z] = stream.astype(jnp.bfloat16)
    all_gather(1, 0, H)
    in_rows(1, NX)
    pltpu.make_async_copy(NX, result, out_sem.at[6]).start()

    for layer in range(2):
        wait_bytes(A.at[layer, pl.ds(0, T - 1)], a_send.at[layer])
        wait_bytes(B.at[layer, pl.ds(0, Z - 1)], b_send.at[layer])
        wait_bytes(C.at[2 * layer], c_send.at[layer])
        wait_bytes(C.at[2 * layer, :, pl.ds(0, X - 1)], c_send.at[layer])
        wait_bytes(DN.at[layer, :, pl.ds(0, (T - 1) * dcol)], d_send.at[layer])
        wait_bytes(SL.at[layer], rl_send.at[layer])
        wait_bytes(SR.at[layer, pl.ds(0, H - 1)], rr_send.at[layer])
        wait_bytes(N.at[layer, pl.ds(0, H)], gr_send.at[layer])
        wait_bytes(N.at[layer, pl.ds(0, H - 1)], gl_send.at[layer])
    for k, (src, dst) in enumerate(
        ((C.at[0], sg1), (C.at[1], su1), (C.at[2], sg2), (C.at[3], su2), (DN.at[0], sd1), (DN.at[1], sd2), (NX, result))
    ):
        pltpu.make_async_copy(src, dst, out_sem.at[k]).wait()


def fold(gain, weight):
    return (gain[:, None] * weight).astype(jnp.bfloat16)


def on_device(Z, T, prompt, g1, wg1, wu1, wd1, g2, wg2, wu2, wd2):
    bf = jnp.bfloat16
    folded = jnp.stack([fold(g1, wg1), fold(g1, wu1), fold(g2, wg2), fold(g2, wu2)])
    downs = jnp.stack([wd1.astype(bf), wd2.astype(bf)])
    X = T // CORES
    H = Z // 2
    rows, width = wg1.shape
    hid = wd1.shape[0]
    tok, D = prompt.shape
    own = tok // Z
    rq = rows // X
    served = jax.ShapeDtypeStruct((Z, X, rq, hid), bf)
    down = jax.ShapeDtypeStruct((hid, D), bf)
    dma = pltpu.SemaphoreType.DMA
    ring = (2, H, 2 * own, D // 2)
    outs = pl.pallas_call(
        functools.partial(kernel, Z, T),
        out_shape=(jax.ShapeDtypeStruct((tok, D), bf), served, served, down, served, served, down),
        in_specs=[pl.BlockSpec(memory_space=pltpu.VMEM)] * 3,
        out_specs=(pl.BlockSpec(memory_space=pl.ANY),) * 7,
        scratch_shapes=[
            pltpu.VMEM((2, T, rq, width), bf),
            pltpu.VMEM((2, Z, rq, hid), bf),
            pltpu.VMEM((4, Z, X, rq, hid), bf),
            pltpu.VMEM((2, hid, D), bf),
            pltpu.VMEM((tok, D), bf),
            pltpu.VMEM((Z, 2 * own, D // 2), jnp.float32),
            pltpu.VMEM(ring, bf), pltpu.VMEM(ring, bf), pltpu.VMEM(ring, bf), pltpu.VMEM(ring, bf),
            pltpu.VMEM((2, Z, 2 * own, D // 2), bf),
            dma((2,)), dma((2,)), dma((2,)), dma((2,)), dma((2,)), dma((2, X - 1)), dma((2,)), dma((2,)), dma((2,)),
            dma((2,)), dma((2, H)), dma((2,)), dma((2, H)), dma((2,)), dma((2, H)), dma((2,)), dma((2, H)),
            dma((2,)), dma((7,)),
        ],
        compiler_params=pltpu.CompilerParams(collective_id=0, has_side_effects=True),
        name="handoff",
    )(prompt, folded, downs)
    flat = lambda a: a.reshape(-1, hid)
    return (outs[0], flat(outs[1]), flat(outs[2]), outs[3], flat(outs[4]), flat(outs[5]), outs[6])


def solution(mesh):
    return jax.shard_map(
        functools.partial(on_device, mesh.shape["fs"], mesh.shape["tp"]),
        mesh=mesh,
        in_specs=(
            P(("grp", "tp"), None),
            P("fs"),
            P("fs", "tp"),
            P("fs", "tp"),
            P("fs", "tp"),
            P("fs"),
            P("fs", "tp"),
            P("fs", "tp"),
            P("fs", "tp"),
        ),
        out_specs=(
            P(("grp", "tp"), None),
            P("grp", "fs"),
            P("grp", "fs"),
            P("fs", "grp"),
            P("grp", "fs"),
            P("grp", "fs"),
            P("fs", "grp"),
        ),
        check_vma=False,
    )
```

```python
import functools

import jax
import jax.numpy as jnp
from jax import lax
from jax.experimental import pallas as pl
from jax.experimental.pallas import tpu as pltpu
from jax.sharding import PartitionSpec as P

EPS = 1e-06
CORES = 2
MESH = pl.DeviceIdType.MESH
HOPS = (2, 4, 4, 4)


def rcopy(src, dst, send_sem, recv_sem, **where):
    return pltpu.make_async_remote_copy(
        src_ref=src, dst_ref=dst, send_sem=send_sem, recv_sem=recv_sem,
        device_id=where, device_id_type=MESH,
    )


def wait_bytes(ref, sem):
    pltpu.make_async_copy(ref, ref, sem).wait()


def kernel(
    Z, T,
    prompt, folded, downs,
    result, sg1, su1, sd1, sg2, su2, sd2,
    A, B, C, DN, NX, part, R, S, N,
    a_send, a_recv, b_send, b_recv, c_send, c_recv, p_recv, d_send, d_recv,
    r_send, r_recv, g_send, g_recv,
    loc, out_sem,
):
    z = lax.axis_index("fs")
    t = lax.axis_index("tp")
    X = T // CORES
    x, c = t // CORES, t % CORES
    H = Z // 2
    mats, rows, width = folded.shape
    rq = rows // X
    hid = DN.shape[1]
    zper = width // hid
    dcol = downs.shape[2]
    tok, D = NX.shape
    own = tok // Z
    half = D // 2
    partner = t + 1 - 2 * c

    barrier = pltpu.get_barrier_semaphore()

    @pl.loop(1, Z)
    def _(k):
        pl.semaphore_signal(barrier, inc=1, device_id={"fs": lax.rem(z + k, Z)}, device_id_type=MESH)

    @pl.loop(1, T)
    def _(k):
        pl.semaphore_signal(barrier, inc=1, device_id={"tp": lax.rem(t + k, T)}, device_id_type=MESH)

    pl.semaphore_wait(barrier, Z + T - 2)

    def slice_of(layer, tt):
        return folded.at[2 * layer + tt // X, pl.ds(pl.multiple_of(lax.rem(tt, X) * rq, rq), rq), :]

    for layer in range(2):
        @pl.loop(1, T)
        def _(k):
            tt = lax.rem(t + k, T)
            rcopy(slice_of(layer, tt), A.at[layer, t], a_send.at[layer], a_recv.at[layer], tp=tt).start()

        pltpu.make_async_copy(slice_of(layer, t), A.at[layer, t], a_recv.at[layer]).start()

    for layer in range(2):
        mine = DN.at[layer, :, pl.ds(pl.multiple_of(t * dcol, dcol), dcol)]

        @pl.loop(1, T)
        def _(k):
            tt = lax.rem(t + k, T)
            rcopy(downs.at[layer], mine, d_send.at[layer], d_recv.at[layer], tp=tt).start()

        pltpu.make_async_copy(downs.at[layer], mine, d_recv.at[layer]).start()

    @pl.loop(0, tok // 16)
    def _(i):
        r = pl.ds(pl.multiple_of(i * 16, 16), 16)
        v = prompt[r, :].astype(jnp.float32)
        NX[r, :] = (v * lax.rsqrt(jnp.mean(v * v, axis=-1, keepdims=True) + EPS)).astype(jnp.bfloat16)

    pair = prompt[pl.ds(pl.multiple_of((z // 2) * 16, 16), 16), :].astype(jnp.float32)
    stream = jnp.where(lax.rem(z, 2) == 0, pair[:own], pair[own:])
    stream = jnp.concatenate([stream[:, :half], stream[:, half:]], axis=0)

    def block_for(layer, zz):
        return A.at[layer, zz // zper, :, pl.ds(pl.multiple_of(lax.rem(zz, zper) * hid, hid), hid)]

    def spread(layer, k):
        @pl.when(k < H)
        def _():
            zz = lax.rem(z + Z - k, Z)
            rcopy(block_for(layer, zz), B.at[layer, z], b_send.at[layer], b_recv.at[layer], fs=zz).start()

        zz = lax.rem(z + k, Z)
        rcopy(block_for(layer, zz), B.at[layer, z], b_send.at[layer], b_recv.at[layer], fs=zz).start()

    def spread_own(layer):
        pltpu.make_async_copy(block_for(layer, z), B.at[layer, z], b_recv.at[layer]).start()

    def rows_of(layer, tt):
        return C.at[2 * layer + tt // X, :, lax.rem(tt, X)]

    def gather_start(layer):
        wait_bytes(B.at[layer], b_recv.at[layer])
        for k in range(1, X):
            tt = lax.rem(t + CORES * k, T)
            rcopy(B.at[layer], rows_of(layer, t), c_send.at[layer], c_recv.at[layer, k - 1], tp=tt).start()
        rcopy(B.at[layer], rows_of(layer, t), c_send.at[layer], p_recv.at[layer], tp=partner).start()
        pltpu.make_async_copy(B.at[layer], rows_of(layer, t), loc.at[layer]).start()

    def gather_pass(layer):
        for k in (1, 3, 2) if X == 4 else range(1, X):
            tt = lax.rem(t + T - CORES * k, T)
            pltpu.make_async_copy(rows_of(layer, tt), rows_of(layer, tt), c_recv.at[layer, k - 1]).wait()
            rcopy(rows_of(layer, tt), rows_of(layer, tt), c_send.at[layer], p_recv.at[layer], tp=partner).start()

    def gather_end(layer):
        wait_bytes(C.at[2 * layer], p_recv.at[layer])
        pltpu.make_async_copy(B.at[layer], B.at[layer], loc.at[layer]).wait()
        for m, out in enumerate(((sg1, su1), (sg2, su2))[layer]):
            pltpu.make_async_copy(C.at[2 * layer + m], out, out_sem.at[2 * layer + m]).start()

    def partial_sums(layer):
        normed = NX[...]
        gate = jnp.dot(normed, C[2 * layer].reshape(D, hid), preferred_element_type=jnp.float32)
        up = jnp.dot(normed, C[2 * layer + 1].reshape(D, hid), preferred_element_type=jnp.float32)
        hidden = (gate / (1.0 + jnp.exp(-gate)) * up).astype(jnp.bfloat16)
        wait_bytes(DN.at[layer], d_recv.at[layer])
        pltpu.make_async_copy(DN.at[layer], (sd1, sd2)[layer], out_sem.at[4 + layer]).start()
        for h in range(2):
            got = jnp.dot(hidden, DN[layer, :, h * half:(h + 1) * half], preferred_element_type=jnp.float32)
            part[:, h * own:(h + 1) * own, :] = got.reshape(Z, own, half)

    reach = (H, H - 1)

    def at(side, m):
        return lax.rem(z + (Z - m if side == 0 else m), Z)

    def reduce_scatter(layer, K, beside):
        def send(side, m, i):
            rcopy(
                S.at[layer, side, m - 1], R.at[layer, side, m - 1],
                r_send.at[layer, side], r_recv.at[layer, side, m - 1], fs=at(side, i),
            ).start()

        def arrived(side, m):
            slot = R.at[layer, side, m - 1]
            pltpu.make_async_copy(slot, slot, r_recv.at[layer, side, m - 1]).wait()
            return R[layer, side, m - 1].astype(jnp.float32)

        def raws(side, g, static=True):
            for i in range(K, 0, -1):
                m = g * K + i
                if static and m > reach[side]:
                    continue
                if i == K and not (static and m + 1 > reach[side]):
                    continue
                S[layer, side, m - 1] = part[at(side, m)].astype(jnp.bfloat16)
                send(side, m, i)

        def node(side, j, static=True):
            acc = part[at(side, j * K)]
            for i in range(1, K + 1):
                if static and j * K + i > reach[side]:
                    continue
                acc = acc + arrived(side, j * K + i)
            S[layer, side, j * K - 1] = acc.astype(jnp.bfloat16)
            send(side, j * K, K)

        steps = [-(-M // K) for M in reach]
        low = min(steps) - 1
        for side in range(2):
            raws(side, steps[side] - 1)
        for j in range(max(steps) - 1, max(low, 1) - 1, -1):
            for side in range(2):
                if j < steps[side]:
                    node(side, j)
                    raws(side, j - 1)
        beside(0)

        @pl.loop(1, low)
        def _(s):
            for side in range(2):
                node(side, low - s, False)
                raws(side, low - s - 1, False)
            beside(s)

        total = part[z]
        for i in range(1, K + 1):
            for side in range(2):
                total = total + arrived(side, i)
        return total

    span = (H - 1, H)

    def all_gather(layer, K, beside):
        def arrived(side, m):
            slot = N.at[layer, at(side, m)]
            pltpu.make_async_copy(slot, slot, g_recv.at[layer, side, m - 1]).wait()

        def step(side, s, static=True):
            for h in range(K, 0, -1):
                if static and s * K + h > span[side]:
                    continue
                slot = N.at[layer, at(side, s * K)]
                rcopy(
                    slot, slot, g_send.at[layer, side], g_recv.at[layer, side, s * K + h - 1],
                    fs=at(1 - side, h),
                ).start()

        steps = [-(-M // K) for M in span]
        low = min(steps) - 1
        for side in range(2):
            step(side, 0)

        @pl.loop(1, low)
        def _(s):
            for side in range(2):
                arrived(side, s * K)
                step(side, s, False)

        for s in range(max(low, 1), max(steps)):
            for side in range(2):
                if s < steps[side]:
                    arrived(side, s * K)
                    step(side, s)
        beside()
        for side in range(2):
            for g in range(steps[side]):
                for i in range(1, K + 1):
                    m = g * K + i
                    if m <= span[side] and not (i == K and g < steps[side] - 1):
                        arrived(side, m)

    def in_rows(layer, out):
        @pl.loop(0, Z // 2)
        def _(i):
            a = N[layer, 2 * i].astype(jnp.float32)
            b = N[layer, 2 * i + 1].astype(jnp.float32)
            r = pl.ds(pl.multiple_of(i * 16, 16), 16)
            out[r, :half] = jnp.concatenate([a[:own], b[:own]], axis=0).astype(jnp.bfloat16)
            out[r, half:] = jnp.concatenate([a[own:], b[own:]], axis=0).astype(jnp.bfloat16)

    wait_bytes(A.at[0], a_recv.at[0])
    spread_own(0)

    @pl.loop(0, H)
    def _(i):
        spread(0, H - i)

    gather_start(0)
    gather_pass(0)
    gather_end(0)
    partial_sums(0)

    wait_bytes(A.at[1], a_recv.at[1])
    spread_own(1)
    K = HOPS[0]
    rounds = max(-(-(H - 1) // K) - 1, 1)

    def spread_some(s):
        for i in range(-(-H // rounds)):
            k = H - s * -(-H // rounds) - i
            pl.when(k > 0)(lambda: spread(1, k))

    total = reduce_scatter(0, K, spread_some)
    stream = stream + 0.5 * total
    mean = jnp.sum(stream * stream, axis=-1, keepdims=True)
    mean = (mean[:own] + mean[own:]) / D
    mean = jnp.concatenate([mean, mean], axis=0)
    N[0, z] = (stream * lax.rsqrt(mean + EPS)).astype(jnp.bfloat16)
    gather_start(1)
    all_gather(0, HOPS[1], lambda: gather_pass(1))
    in_rows(0, NX)
    gather_end(1)
    partial_sums(1)
    total = reduce_scatter(1, HOPS[2], lambda s: None)
    stream = stream + 0.5 * total
    N[1, z] = stream.astype(jnp.bfloat16)
    all_gather(1, HOPS[3], lambda: None)
    in_rows(1, NX)
    pltpu.make_async_copy(NX, result, out_sem.at[6]).start()

    for layer in range(2):
        wait_bytes(A.at[layer, pl.ds(0, T - 1)], a_send.at[layer])
        wait_bytes(B.at[layer, pl.ds(0, Z - 1)], b_send.at[layer])
        wait_bytes(C.at[2 * layer], c_send.at[layer])
        wait_bytes(C.at[2 * layer, :, pl.ds(0, X - 1)], c_send.at[layer])
        wait_bytes(DN.at[layer, :, pl.ds(0, (T - 1) * dcol)], d_send.at[layer])
        for side in range(2):
            wait_bytes(S.at[layer, side, pl.ds(0, reach[side])], r_send.at[layer, side])
            wait_bytes(N.at[layer, pl.ds(0, span[side])], g_send.at[layer, side])
    for k, (src, dst) in enumerate(
        ((C.at[0], sg1), (C.at[1], su1), (C.at[2], sg2), (C.at[3], su2), (DN.at[0], sd1), (DN.at[1], sd2), (NX, result))
    ):
        pltpu.make_async_copy(src, dst, out_sem.at[k]).wait()


def fold(gain, weight):
    return (gain[:, None] * weight).astype(jnp.bfloat16)


def on_device(Z, T, prompt, g1, wg1, wu1, wd1, g2, wg2, wu2, wd2):
    bf = jnp.bfloat16
    folded = jnp.stack([fold(g1, wg1), fold(g1, wu1), fold(g2, wg2), fold(g2, wu2)])
    downs = jnp.stack([wd1.astype(bf), wd2.astype(bf)])
    X = T // CORES
    H = Z // 2
    rows, width = wg1.shape
    hid = wd1.shape[0]
    tok, D = prompt.shape
    own = tok // Z
    rq = rows // X
    served = jax.ShapeDtypeStruct((Z, X, rq, hid), bf)
    down = jax.ShapeDtypeStruct((hid, D), bf)
    dma = pltpu.SemaphoreType.DMA
    ring = (2, 2, H, 2 * own, D // 2)
    outs = pl.pallas_call(
        functools.partial(kernel, Z, T),
        out_shape=(jax.ShapeDtypeStruct((tok, D), bf), served, served, down, served, served, down),
        in_specs=[pl.BlockSpec(memory_space=pltpu.VMEM)] * 3,
        out_specs=(pl.BlockSpec(memory_space=pl.ANY),) * 7,
        scratch_shapes=[
            pltpu.VMEM((2, T, rq, width), bf),
            pltpu.VMEM((2, Z, rq, hid), bf),
            pltpu.VMEM((4, Z, X, rq, hid), bf),
            pltpu.VMEM((2, hid, D), bf),
            pltpu.VMEM((tok, D), bf),
            pltpu.VMEM((Z, 2 * own, D // 2), jnp.float32),
            pltpu.VMEM(ring, bf), pltpu.VMEM(ring, bf),
            pltpu.VMEM((2, Z, 2 * own, D // 2), bf),
            dma((2,)), dma((2,)), dma((2,)), dma((2,)), dma((2,)), dma((2, X - 1)), dma((2,)), dma((2,)), dma((2,)),
            dma((2, 2)), dma((2, 2, H)), dma((2, 2)), dma((2, 2, H)),
            dma((2,)), dma((7,)),
        ],
        compiler_params=pltpu.CompilerParams(collective_id=0, has_side_effects=True),
        name="handoff",
    )(prompt, folded, downs)
    flat = lambda a: a.reshape(-1, hid)
    return (outs[0], flat(outs[1]), flat(outs[2]), outs[3], flat(outs[4]), flat(outs[5]), outs[6])


def solution(mesh):
    return jax.shard_map(
        functools.partial(on_device, mesh.shape["fs"], mesh.shape["tp"]),
        mesh=mesh,
        in_specs=(
            P(("grp", "tp"), None),
            P("fs"),
            P("fs", "tp"),
            P("fs", "tp"),
            P("fs", "tp"),
            P("fs"),
            P("fs", "tp"),
            P("fs", "tp"),
            P("fs", "tp"),
        ),
        out_specs=(
            P(("grp", "tp"), None),
            P("grp", "fs"),
            P("grp", "fs"),
            P("fs", "grp"),
            P("grp", "fs"),
            P("grp", "fs"),
            P("fs", "grp"),
        ),
        check_vma=False,
    )
```

```python
import functools

import jax
import jax.numpy as jnp
from jax import lax
from jax.experimental import pallas as pl
from jax.experimental.pallas import tpu as pltpu
from jax.sharding import PartitionSpec as P

EPS = 1e-06
VMEM = 67_043_328
CORES = 2
MESH = pl.DeviceIdType.MESH
TREE = (0, 1, 0, 3, 4, 0)


def tree(span):
    K = len(TREE)
    parent = {m: (m - 1) // K * K + TREE[(m - 1) % K] for m in range(1, span + 1)}
    feeds = {a: [m for m in range(span, 0, -1) if parent[m] == a] for a in range(span + 1)}
    starts = [a for a in range(0, span + 1, K) if feeds[a]]
    order = []
    for k in range(len(starts) + 1):
        order += starts[k:k + 1]
        if k:
            order += [a for a in range(starts[k - 1] + 1, starts[k - 1] + K) if feeds.get(a)]
    return parent, feeds, order


def alternate(*lists):
    return [(side, step[k]) for k in range(max(map(len, lists))) for side, step in enumerate(lists) if k < len(step)]


def rcopy(src, dst, send_sem, recv_sem, **where):
    return pltpu.make_async_remote_copy(
        src_ref=src, dst_ref=dst, send_sem=send_sem, recv_sem=recv_sem,
        device_id=where, device_id_type=MESH,
    )


def wait_bytes(ref, sem):
    pltpu.make_async_copy(ref, ref, sem).wait()


def kernel(
    Z, T,
    prompt_in, g1, wg1, wu1, wd1, g2, wg2, wu2, wd2,
    C, DN, NX,
    prompt, gains, wide, tall, folded, downs,
    A, B, part, R, S, N,
    a_send, a_recv, b_send, b_recv, c_send, c_recv, p_recv, d_send, d_recv,
    r_send, r_recv, g_send, g_recv,
    loc, load_sem,
):
    z = lax.axis_index("fs")
    t = lax.axis_index("tp")
    X = T // CORES
    x, c = t // CORES, t % CORES
    H = Z // 2
    mats, rows, width = folded.shape
    rq = rows // X
    hid = DN.shape[1]
    zper = width // hid
    dcol = downs.shape[2]
    tok, D = NX.shape
    own = tok // Z
    half = D // 2
    partner = t + 1 - 2 * c

    loads = [(prompt_in, prompt)]
    for layer, (g, wg, wu, wd) in enumerate(((g1, wg1, wu1, wd1), (g2, wg2, wu2, wd2))):
        loads += [(g, gains.at[layer]), (wg, wide.at[2 * layer]), (wu, wide.at[2 * layer + 1]), (wd, tall.at[layer])]
    loads = [pltpu.make_async_copy(src, dst, load_sem.at[k]) for k, (src, dst) in enumerate(loads)]
    for k in (1, 2, 3, 5, 6, 7, 4, 8, 0):
        loads[k].start()

    barrier = pltpu.get_barrier_semaphore()

    @pl.loop(1, Z)
    def _(k):
        pl.semaphore_signal(barrier, inc=1, device_id={"fs": lax.rem(z + k, Z)}, device_id_type=MESH)

    @pl.loop(1, T)
    def _(k):
        pl.semaphore_signal(barrier, inc=1, device_id={"tp": lax.rem(t + k, T)}, device_id_type=MESH)

    for layer in range(2):
        for k in range(1, 4):
            loads[4 * layer + k].wait()
        diagonal = lax.broadcasted_iota(jnp.int32, (rows, rows), 0) == lax.broadcasted_iota(jnp.int32, (rows, rows), 1)
        gain = jnp.sum(jnp.where(diagonal, gains[layer], 0.0), axis=1, keepdims=True)
        for m in (2 * layer, 2 * layer + 1):
            folded[m] = (gain * wide[m]).astype(jnp.bfloat16)
    for layer in range(2):
        loads[4 * layer + 4].wait()
        downs[layer] = tall[layer].astype(jnp.bfloat16)
    loads[0].wait()

    @pl.loop(0, tok // 16)
    def _(i):
        r = pl.ds(pl.multiple_of(i * 16, 16), 16)
        v = prompt[r, :].astype(jnp.float32)
        NX[r, :] = (v * lax.rsqrt(jnp.mean(v * v, axis=-1, keepdims=True) + EPS)).astype(jnp.bfloat16)

    pair = prompt[pl.ds(pl.multiple_of((z // 2) * 16, 16), 16), :].astype(jnp.float32)
    stream = jnp.where(lax.rem(z, 2) == 0, pair[:own], pair[own:])
    stream = jnp.concatenate([stream[:, :half], stream[:, half:]], axis=0)

    pl.semaphore_wait(barrier, Z + T - 2)

    pend = {}

    def due(name, ref, sem):
        pend[name] = lambda: wait_bytes(ref, sem)

    def settle(name):
        pend.pop(name)()

    def finish():
        for name in list(pend):
            settle(name)

    def slice_of(layer, tt):
        return folded.at[2 * layer + tt // X, pl.ds(pl.multiple_of(lax.rem(tt, X) * rq, rq), rq), :]

    for layer in range(2):
        @pl.loop(1, T)
        def _(k):
            tt = lax.rem(t + k, T)
            rcopy(slice_of(layer, tt), A.at[layer, t], a_send.at[layer], a_recv.at[layer], tp=tt).start()

        pltpu.make_async_copy(slice_of(layer, t), A.at[layer, t], a_recv.at[layer]).start()
        due(f"A{layer}", A.at[layer], a_recv.at[layer])
        due(f"As{layer}", A.at[layer, pl.ds(0, T - 1)], a_send.at[layer])

    for layer in range(2):
        mine = DN.at[layer, :, pl.ds(pl.multiple_of(t * dcol, dcol), dcol)]

        @pl.loop(1, T)
        def _(k):
            tt = lax.rem(t + k, T)
            rcopy(downs.at[layer], mine, d_send.at[layer], d_recv.at[layer], tp=tt).start()

        pltpu.make_async_copy(downs.at[layer], mine, d_recv.at[layer]).start()
        due(f"D{layer}", DN.at[layer], d_recv.at[layer])
        due(f"Ds{layer}", DN.at[layer, :, pl.ds(0, (T - 1) * dcol)], d_send.at[layer])

    def block_for(layer, zz):
        return A.at[layer, zz // zper, :, pl.ds(pl.multiple_of(lax.rem(zz, zper) * hid, hid), hid)]

    def spread(layer, k):
        @pl.when(k < H)
        def _():
            zz = lax.rem(z + Z - k, Z)
            rcopy(block_for(layer, zz), B.at[layer, z], b_send.at[layer], b_recv.at[layer], fs=zz).start()

        zz = lax.rem(z + k, Z)
        rcopy(block_for(layer, zz), B.at[layer, z], b_send.at[layer], b_recv.at[layer], fs=zz).start()

    def spread_own(layer):
        pltpu.make_async_copy(block_for(layer, z), B.at[layer, z], b_recv.at[layer]).start()
        due(f"B{layer}", B.at[layer], b_recv.at[layer])
        due(f"Bs{layer}", B.at[layer, pl.ds(0, Z - 1)], b_send.at[layer])

    def rows_of(layer, tt):
        return C.at[2 * layer + tt // X, :, lax.rem(tt, X)]

    def gather_start(layer):
        settle(f"B{layer}")
        for k in range(1, X):
            tt = lax.rem(t + CORES * k, T)
            rcopy(B.at[layer], rows_of(layer, t), c_send.at[layer], c_recv.at[layer, k - 1], tp=tt).start()
        rcopy(B.at[layer], rows_of(layer, t), c_send.at[layer], p_recv.at[layer], tp=partner).start()
        pltpu.make_async_copy(B.at[layer], rows_of(layer, t), loc.at[layer]).start()
        due(f"Cp{layer}", C.at[2 * layer], p_recv.at[layer])
        due(f"Co{layer}", B.at[layer], loc.at[layer])
        due(f"Cs{layer}", C.at[2 * layer], c_send.at[layer])
        due(f"Ct{layer}", C.at[2 * layer, :, pl.ds(0, X - 1)], c_send.at[layer])

    def gather_pass(layer):
        for k in (1, 3, 2) if X == 4 else range(1, X):
            tt = lax.rem(t + T - CORES * k, T)
            pltpu.make_async_copy(rows_of(layer, tt), rows_of(layer, tt), c_recv.at[layer, k - 1]).wait()
            rcopy(rows_of(layer, tt), rows_of(layer, tt), c_send.at[layer], p_recv.at[layer], tp=partner).start()

    def gather_end(layer):
        settle(f"Cp{layer}")
        settle(f"Co{layer}")

    def partial_sums(layer):
        normed = NX[...]
        gate = jnp.dot(normed, C[2 * layer].reshape(D, hid), preferred_element_type=jnp.float32)
        up = jnp.dot(normed, C[2 * layer + 1].reshape(D, hid), preferred_element_type=jnp.float32)
        hidden = (gate / (1.0 + jnp.exp(-gate)) * up).astype(jnp.bfloat16)
        settle(f"D{layer}")
        for h in range(2):
            got = jnp.dot(hidden, DN[layer, :, h * half:(h + 1) * half], preferred_element_type=jnp.float32)
            part[:, h * own:(h + 1) * own, :] = got.reshape(Z, own, half)

    reach = (H, H - 1)

    def at(side, m):
        return lax.rem(z + (Z - m if side == 0 else m), Z)

    def reduce_scatter(layer):
        trees = [tree(M) for M in reach]

        def send(side, m, value):
            S[layer, side, m - 1] = value.astype(jnp.bfloat16)
            rcopy(
                S.at[layer, side, m - 1], R.at[layer, side, m - 1],
                r_send.at[layer, side], r_recv.at[layer, side, m - 1], fs=at(side, m - trees[side][0][m]),
            ).start()

        def gathered(side, a):
            acc = part[at(side, a)]
            for m in reversed(trees[side][1][a]):
                slot = R.at[layer, side, m - 1]
                pltpu.make_async_copy(slot, slot, r_recv.at[layer, side, m - 1]).wait()
                acc = acc + R[layer, side, m - 1].astype(jnp.float32)
            return acc

        def own_sums(side, k):
            _, feeds, order = trees[side]
            nodes = order[::-1]
            if k < len(nodes):
                for m in feeds[nodes[k]]:
                    if not feeds[m]:
                        send(side, m, part[at(side, m)])

        lead = 2
        for k in range(lead):
            for side in range(2):
                own_sums(side, k)
        for side, (k, a) in alternate(*([*enumerate(trees[i][2][::-1])] for i in range(2))):
            if a:
                send(side, a, gathered(side, a))
                own_sums(side, k + lead)
        for side in range(2):
            due(f"Rs{layer}{side}", S.at[layer, side, pl.ds(0, reach[side])], r_send.at[layer, side])
        return gathered(0, 0) + gathered(1, 0) - part[z]

    span = (H - 1, H)

    def all_gather(layer, beside):
        trees = [tree(M) for M in span]

        def arrived(side, m):
            slot = N.at[layer, at(side, m)]
            pltpu.make_async_copy(slot, slot, g_recv.at[layer, side, m - 1]).wait()

        for side, a in alternate(trees[0][2], trees[1][2]):
            if a:
                arrived(side, a)
            for m in trees[side][1][a]:
                slot = N.at[layer, at(side, a)]
                rcopy(
                    slot, slot, g_send.at[layer, side], g_recv.at[layer, side, m - 1], fs=at(1 - side, m - a),
                ).start()
        beside()
        for side in range(2):
            due(f"Gs{layer}{side}", N.at[layer, pl.ds(0, span[side])], g_send.at[layer, side])
            for m in range(1, span[side] + 1):
                if not trees[side][1][m]:
                    arrived(side, m)

    def in_rows(layer, out):
        @pl.loop(0, Z // 2)
        def _(i):
            a = N[layer, 2 * i].astype(jnp.float32)
            b = N[layer, 2 * i + 1].astype(jnp.float32)
            r = pl.ds(pl.multiple_of(i * 16, 16), 16)
            out[r, :half] = jnp.concatenate([a[:own], b[:own]], axis=0).astype(jnp.bfloat16)
            out[r, half:] = jnp.concatenate([a[own:], b[own:]], axis=0).astype(jnp.bfloat16)

    settle("A0")
    spread_own(0)

    @pl.loop(0, H)
    def _(i):
        spread(0, H - i)

    gather_start(0)
    settle("A1")
    spread_own(1)

    @pl.loop(0, H)
    def _(i):
        spread(1, H - i)

    gather_pass(0)
    gather_end(0)
    partial_sums(0)
    total = reduce_scatter(0)
    stream = stream + 0.5 * total
    mean = jnp.sum(stream * stream, axis=-1, keepdims=True)
    mean = (mean[:own] + mean[own:]) / D
    mean = jnp.concatenate([mean, mean], axis=0)
    N[0, z] = (stream * lax.rsqrt(mean + EPS)).astype(jnp.bfloat16)
    gather_start(1)
    all_gather(0, lambda: gather_pass(1))
    in_rows(0, NX)
    gather_end(1)
    partial_sums(1)
    total = reduce_scatter(1)
    stream = stream + 0.5 * total
    N[1, z] = stream.astype(jnp.bfloat16)
    all_gather(1, lambda: None)
    in_rows(1, NX)
    finish()


def put_out(C, DN, NX, result, sg1, su1, sd1, sg2, su2, sd2, sem):
    pairs = ((C.at[0], sg1), (C.at[1], su1), (C.at[2], sg2), (C.at[3], su2), (DN.at[0], sd1), (DN.at[1], sd2), (NX, result))
    copies = [pltpu.make_async_copy(src, dst, sem.at[k]) for k, (src, dst) in enumerate(pairs)]
    for copy in copies:
        copy.start()
    for copy in copies:
        copy.wait()


def on_device(Z, T, prompt, g1, wg1, wu1, wd1, g2, wg2, wu2, wd2):
    bf, f32 = jnp.bfloat16, jnp.float32
    X = T // CORES
    H = Z // 2
    rows, width = wg1.shape
    hid, dcol = wd1.shape
    tok, D = prompt.shape
    own = tok // Z
    rq = rows // X
    served = jax.ShapeDtypeStruct((Z, X, rq, hid), bf)
    down = jax.ShapeDtypeStruct((hid, D), bf)
    dma = pltpu.SemaphoreType.DMA
    ring = (2, 2, H, 2 * own, D // 2)
    anywhere = pl.BlockSpec(memory_space=pl.ANY)
    in_vmem = pl.BlockSpec(memory_space=pltpu.VMEM)
    held = pl.pallas_call(
        functools.partial(kernel, Z, T),
        out_shape=(pltpu.VMEM((4, Z, X, rq, hid), bf), pltpu.VMEM((2, hid, D), bf), pltpu.VMEM((tok, D), bf)),
        in_specs=[anywhere] * 9,
        out_specs=(in_vmem,) * 3,
        scratch_shapes=[
            pltpu.VMEM((tok, D), bf),
            pltpu.VMEM((2, 1, rows), f32),
            pltpu.VMEM((4, rows, width), f32),
            pltpu.VMEM((2, hid, dcol), f32),
            pltpu.VMEM((4, rows, width), bf),
            pltpu.VMEM((2, hid, dcol), bf),
            pltpu.VMEM((2, T, rq, width), bf),
            pltpu.VMEM((2, Z, rq, hid), bf),
            pltpu.VMEM((Z, 2 * own, D // 2), f32),
            pltpu.VMEM(ring, bf), pltpu.VMEM(ring, bf),
            pltpu.VMEM((2, Z, 2 * own, D // 2), bf),
            dma((2,)), dma((2,)), dma((2,)), dma((2,)), dma((2,)), dma((2, X - 1)), dma((2,)), dma((2,)), dma((2,)),
            dma((2, 2)), dma((2, 2, H)), dma((2, 2)), dma((2, 2, H)),
            dma((2,)), dma((9,)),
        ],
        compiler_params=pltpu.CompilerParams(collective_id=0, has_side_effects=True, vmem_limit_bytes=VMEM - 2 * (4 * Z * X * rq * hid + 2 * hid * D + tok * D)),
        name="handoff",
    )(prompt, g1.reshape(1, rows), wg1, wu1, wd1, g2.reshape(1, rows), wg2, wu2, wd2)
    outs = pl.pallas_call(
        put_out,
        out_shape=(jax.ShapeDtypeStruct((tok, D), bf), served, served, down, served, served, down),
        in_specs=[in_vmem] * 3,
        out_specs=(anywhere,) * 7,
        scratch_shapes=[dma((7,))],
        compiler_params=pltpu.CompilerParams(vmem_limit_bytes=8 * 2**20),
        name="put_out",
    )(*held)
    flat = lambda a: a.reshape(-1, hid)
    return (outs[0], flat(outs[1]), flat(outs[2]), outs[3], flat(outs[4]), flat(outs[5]), outs[6])


def solution(mesh):
    return jax.shard_map(
        functools.partial(on_device, mesh.shape["fs"], mesh.shape["tp"]),
        mesh=mesh,
        in_specs=(
            P(("grp", "tp"), None),
            P("fs"),
            P("fs", "tp"),
            P("fs", "tp"),
            P("fs", "tp"),
            P("fs"),
            P("fs", "tp"),
            P("fs", "tp"),
            P("fs", "tp"),
        ),
        out_specs=(
            P(("grp", "tp"), None),
            P("grp", "fs"),
            P("grp", "fs"),
            P("fs", "grp"),
            P("grp", "fs"),
            P("grp", "fs"),
            P("fs", "grp"),
        ),
        check_vma=False,
    )
```

```python
import functools

import jax
import jax.numpy as jnp
from jax import lax
from jax.experimental import pallas as pl
from jax.experimental.pallas import tpu as pltpu
from jax.sharding import PartitionSpec as P

EPS = 1e-06
VMEM = 67_043_328
NEAR = 4
CORES = 2
MESH = pl.DeviceIdType.MESH
TREES = ((0, 0, 0, 0), (0, 1, 0))


def tree(span, shape):
    K = len(shape)
    parent = {m: (m - 1) // K * K + shape[(m - 1) % K] for m in range(1, span + 1)}
    feeds = {a: [m for m in range(span, 0, -1) if parent[m] == a] for a in range(span + 1)}
    starts = [a for a in range(0, span + 1, K) if feeds[a]]
    order = []
    for k in range(len(starts) + 1):
        order += starts[k:k + 1]
        if k:
            order += [a for a in range(starts[k - 1] + 1, starts[k - 1] + K) if feeds.get(a)]
    return parent, feeds, order


def alternate(*lists):
    return [(side, step[k]) for k in range(max(map(len, lists))) for side, step in enumerate(lists) if k < len(step)]


def rcopy(src, dst, send_sem, recv_sem, **where):
    return pltpu.make_async_remote_copy(
        src_ref=src, dst_ref=dst, send_sem=send_sem, recv_sem=recv_sem,
        device_id=where, device_id_type=MESH,
    )


def wait_bytes(ref, sem):
    pltpu.make_async_copy(ref, ref, sem).wait()


def kernel(
    Z, T,
    prompt_in, g1, wg1, wu1, wd1, g2, wg2, wu2, wd2,
    C, DN, NX,
    prompt, gains, wide, tall, folded, downs,
    A, B, part, total, R, S, N,
    a_send, a_recv, b_send, b_recv, c_send, c_recv, p_recv, d_send, d_recv,
    r_send, r_recv, g_send, g_recv,
    loc, load_sem, word,
):
    z = lax.axis_index("fs")
    t = lax.axis_index("tp")
    X = T // CORES
    x, c = t // CORES, t % CORES
    H = Z // 2
    mats, rows, width = folded.shape
    rq = rows // X
    hid = DN.shape[1]
    zper = width // hid
    dcol = downs.shape[2]
    tok, D = NX.shape
    own = tok // Z
    half = D // 2
    partner = t + 1 - 2 * c

    loads = [(prompt_in, prompt)]
    for layer, (g, wg, wu, wd) in enumerate(((g1, wg1, wu1, wd1), (g2, wg2, wu2, wd2))):
        loads += [(g, gains.at[layer]), (wg, wide.at[2 * layer]), (wu, wide.at[2 * layer + 1]), (wd, tall.at[layer])]
    loads = [pltpu.make_async_copy(src, dst, load_sem.at[k]) for k, (src, dst) in enumerate(loads)]
    for k in (1, 2, 3, 5, 6, 7, 4, 8, 0):
        loads[k].start()

    barrier = pltpu.get_barrier_semaphore()

    def near(r):
        return [{"fs": lax.rem(z + k, Z)} for k in (r, Z - r)]

    first = sorted({k for r in range(1, NEAR + 1) for k in (r, Z - r)})

    for where in [{"fs": lax.rem(z + k, Z)} for k in first] + [{"tp": lax.rem(t + k, T)} for k in range(1, T)]:
        pl.semaphore_signal(barrier, inc=1, device_id=where, device_id_type=MESH)

    for layer in range(2):
        for k in range(1, 4):
            loads[4 * layer + k].wait()
        diagonal = lax.broadcasted_iota(jnp.int32, (rows, rows), 0) == lax.broadcasted_iota(jnp.int32, (rows, rows), 1)
        gain = jnp.sum(jnp.where(diagonal, gains[layer], 0.0), axis=1, keepdims=True)
        for m in (2 * layer, 2 * layer + 1):
            folded[m] = (gain * wide[m]).astype(jnp.bfloat16)
    for layer in range(2):
        loads[4 * layer + 4].wait()
        downs[layer] = tall[layer].astype(jnp.bfloat16)
    pl.semaphore_wait(barrier, len(first) + T - 1)

    radii = [NEAR << k for k in range(H.bit_length()) if NEAR << k < H]

    def tell(k):
        for where in near(radii[k]):
            pl.semaphore_signal(word.at[k], inc=1, device_id=where, device_id_type=MESH)

    if radii:
        tell(0)

    pend = {}

    def due(name, ref, sem):
        pend[name] = lambda: wait_bytes(ref, sem)

    def settle(name):
        pend.pop(name)()

    def finish():
        for name in list(pend):
            settle(name)

    def slice_of(layer, tt):
        return folded.at[2 * layer + tt // X, pl.ds(pl.multiple_of(lax.rem(tt, X) * rq, rq), rq), :]

    for layer in range(2):
        @pl.loop(1, T)
        def _(k):
            tt = lax.rem(t + k, T)
            rcopy(slice_of(layer, tt), A.at[layer, t], a_send.at[layer], a_recv.at[layer], tp=tt).start()

        pltpu.make_async_copy(slice_of(layer, t), A.at[layer, t], a_recv.at[layer]).start()
        due(f"A{layer}", A.at[layer], a_recv.at[layer])
        due(f"As{layer}", A.at[layer, pl.ds(0, T - 1)], a_send.at[layer])

    for layer in range(2):
        mine = DN.at[layer, :, pl.ds(pl.multiple_of(t * dcol, dcol), dcol)]

        @pl.loop(1, T)
        def _(k):
            tt = lax.rem(t + k, T)
            rcopy(downs.at[layer], mine, d_send.at[layer], d_recv.at[layer], tp=tt).start()

        pltpu.make_async_copy(downs.at[layer], mine, d_recv.at[layer]).start()
        due(f"D{layer}", DN.at[layer], d_recv.at[layer])
        due(f"Ds{layer}", DN.at[layer, :, pl.ds(0, (T - 1) * dcol)], d_send.at[layer])

    loads[0].wait()

    @pl.loop(0, tok // 16)
    def _(i):
        r = pl.ds(pl.multiple_of(i * 16, 16), 16)
        v = prompt[r, :].astype(jnp.float32)
        NX[r, :] = (v * lax.rsqrt(jnp.mean(v * v, axis=-1, keepdims=True) + EPS)).astype(jnp.bfloat16)

    pair = prompt[pl.ds(pl.multiple_of((z // 2) * 16, 16), 16), :].astype(jnp.float32)
    stream = jnp.where(lax.rem(z, 2) == 0, pair[:own], pair[own:])
    stream = jnp.concatenate([stream[:, :half], stream[:, half:]], axis=0)

    for k in range(len(radii)):
        pl.semaphore_wait(word.at[k], 2)
        if k + 1 < len(radii):
            tell(k + 1)

    def block_for(layer, zz):
        return A.at[layer, zz // zper, :, pl.ds(pl.multiple_of(lax.rem(zz, zper) * hid, hid), hid)]

    def spread(layer, k):
        @pl.when(k < H)
        def _():
            zz = lax.rem(z + Z - k, Z)
            rcopy(block_for(layer, zz), B.at[layer, z], b_send.at[layer], b_recv.at[layer], fs=zz).start()

        zz = lax.rem(z + k, Z)
        rcopy(block_for(layer, zz), B.at[layer, z], b_send.at[layer], b_recv.at[layer], fs=zz).start()

    def spread_own(layer):
        pltpu.make_async_copy(block_for(layer, z), B.at[layer, z], b_recv.at[layer]).start()
        due(f"B{layer}", B.at[layer], b_recv.at[layer])
        due(f"Bs{layer}", B.at[layer, pl.ds(0, Z - 1)], b_send.at[layer])

    def rows_of(layer, tt):
        return C.at[2 * layer + tt // X, :, lax.rem(tt, X)]

    around = X == 4

    def half_of(layer, tt, h):
        return C.at[2 * layer + tt // X, pl.ds(h * H, H), lax.rem(tt, X)]

    def gather_start(layer):
        settle(f"B{layer}")
        for k in (1, X - 1) if around else range(1, X):
            tt = lax.rem(t + CORES * k, T)
            rcopy(B.at[layer], rows_of(layer, t), c_send.at[layer], c_recv.at[layer, k], tp=tt).start()
        rcopy(B.at[layer], rows_of(layer, t), c_send.at[layer], p_recv.at[layer], tp=partner).start()
        pltpu.make_async_copy(B.at[layer], rows_of(layer, t), loc.at[layer]).start()
        due(f"Cp{layer}", C.at[2 * layer], p_recv.at[layer])
        due(f"Co{layer}", B.at[layer], loc.at[layer])
        due(f"Cs{layer}", C.at[2 * layer], c_send.at[layer])
        due(f"Ct{layer}", C.at[2 * layer, :, pl.ds(0, X - 1)], c_send.at[layer])

    def gather_pass(layer):
        for k in (1, X - 1, 2) if around else range(1, X):
            tt = lax.rem(t + T - CORES * k, T)
            rows_tt = rows_of(layer, tt)
            if around and k == 2:
                for h in (0, 2):
                    piece = half_of(layer, tt, h // 2)
                    pltpu.make_async_copy(piece, piece, c_recv.at[layer, h]).wait()
            else:
                pltpu.make_async_copy(rows_tt, rows_tt, c_recv.at[layer, k]).wait()
                if around:
                    h = 0 if k == 1 else 1
                    piece = half_of(layer, tt, h)
                    on = lax.rem(t + (CORES if k == 1 else T - CORES), T)
                    rcopy(piece, piece, c_send.at[layer], c_recv.at[layer, 2 * h], tp=on).start()
            rcopy(rows_tt, rows_tt, c_send.at[layer], p_recv.at[layer], tp=partner).start()

    def gather_end(layer):
        settle(f"Cp{layer}")
        settle(f"Co{layer}")

    def partial_sums(layer):
        normed = NX[...]
        gate = jnp.dot(normed, C[2 * layer].reshape(D, hid), preferred_element_type=jnp.float32)
        up = jnp.dot(normed, C[2 * layer + 1].reshape(D, hid), preferred_element_type=jnp.float32)
        hidden = (gate / (1.0 + jnp.exp(-gate)) * up).astype(jnp.bfloat16)
        settle(f"D{layer}")
        for h in range(2):
            got = jnp.dot(hidden, DN[layer, :, h * half:(h + 1) * half], preferred_element_type=jnp.float32)
            part[:, h * own:(h + 1) * own, :] = got.reshape(Z, own, half)

    reach = (H, H - 1)

    def at(side, m):
        return lax.rem(z + (Z - m if side == 0 else m), Z)

    def reduce_along(layer, shape):
        trees = [tree(M, shape) for M in reach]

        def send(side, m, value):
            S[layer, side, m - 1] = value.astype(jnp.bfloat16)
            rcopy(
                S.at[layer, side, m - 1], R.at[layer, side, m - 1],
                r_send.at[layer, side], r_recv.at[layer, side, m - 1], fs=at(side, m - trees[side][0][m]),
            ).start()

        def gathered(side, a):
            acc = part[at(side, a)]
            for m in reversed(trees[side][1][a]):
                slot = R.at[layer, side, m - 1]
                pltpu.make_async_copy(slot, slot, r_recv.at[layer, side, m - 1]).wait()
                acc = acc + R[layer, side, m - 1].astype(jnp.float32)
            return acc

        def own_sums(side, k):
            _, feeds, order = trees[side]
            nodes = order[::-1]
            if k < len(nodes):
                for m in feeds[nodes[k]]:
                    if not feeds[m]:
                        send(side, m, part[at(side, m)])

        lead = 2
        for k in range(lead):
            for side in range(2):
                own_sums(side, k)
        for side, (k, a) in alternate(*([*enumerate(trees[i][2][::-1])] for i in range(2))):
            if a:
                send(side, a, gathered(side, a))
                own_sums(side, k + lead)
        total[...] = gathered(0, 0) + gathered(1, 0) - part[z]

    def reduce_scatter(layer):
        for core, shape in enumerate(TREES):
            pl.when(c == core)(functools.partial(reduce_along, layer, shape))
        for side in range(2):
            due(f"Rs{layer}{side}", S.at[layer, side, pl.ds(0, reach[side])], r_send.at[layer, side])
        return total[...]

    span = (H - 1, H)

    def gather_along(layer, shape):
        trees = [tree(M, shape) for M in span]

        def arrived(side, m):
            slot = N.at[layer, at(side, m)]
            pltpu.make_async_copy(slot, slot, g_recv.at[layer, side, m - 1]).wait()

        for side, a in alternate(trees[0][2], trees[1][2]):
            if a:
                arrived(side, a)
            for m in trees[side][1][a]:
                slot = N.at[layer, at(side, a)]
                rcopy(
                    slot, slot, g_send.at[layer, side], g_recv.at[layer, side, m - 1], fs=at(1 - side, m - a),
                ).start()
        for side in range(2):
            for m in range(1, span[side] + 1):
                if not trees[side][1][m]:
                    arrived(side, m)

    def all_gather(layer):
        for core, shape in enumerate(TREES):
            pl.when(c == core)(functools.partial(gather_along, layer, shape))
        for side in range(2):
            due(f"Gs{layer}{side}", N.at[layer, pl.ds(0, span[side])], g_send.at[layer, side])

    def in_rows(layer, out):
        @pl.loop(0, Z // 2)
        def _(i):
            a = N[layer, 2 * i].astype(jnp.float32)
            b = N[layer, 2 * i + 1].astype(jnp.float32)
            r = pl.ds(pl.multiple_of(i * 16, 16), 16)
            out[r, :half] = jnp.concatenate([a[:own], b[:own]], axis=0).astype(jnp.bfloat16)
            out[r, half:] = jnp.concatenate([a[own:], b[own:]], axis=0).astype(jnp.bfloat16)

    settle("A0")
    spread_own(0)

    @pl.loop(0, H)
    def _(i):
        spread(0, H - i)

    gather_start(0)
    settle("A1")
    spread_own(1)

    @pl.loop(0, H)
    def _(i):
        spread(1, H - i)

    gather_pass(0)
    gather_end(0)
    partial_sums(0)
    gather_start(1)
    stream = stream + 0.5 * reduce_scatter(0)
    mean = jnp.sum(stream * stream, axis=-1, keepdims=True)
    mean = (mean[:own] + mean[own:]) / D
    mean = jnp.concatenate([mean, mean], axis=0)
    N[0, z] = (stream * lax.rsqrt(mean + EPS)).astype(jnp.bfloat16)
    gather_pass(1)
    all_gather(0)
    in_rows(0, NX)
    gather_end(1)
    partial_sums(1)
    stream = stream + 0.5 * reduce_scatter(1)
    N[1, z] = stream.astype(jnp.bfloat16)
    all_gather(1)
    in_rows(1, NX)
    finish()


def put_out(C, DN, NX, result, sg1, su1, sd1, sg2, su2, sd2, sem):
    pairs = ((C.at[0], sg1), (C.at[1], su1), (C.at[2], sg2), (C.at[3], su2), (DN.at[0], sd1), (DN.at[1], sd2), (NX, result))
    copies = [pltpu.make_async_copy(src, dst, sem.at[k]) for k, (src, dst) in enumerate(pairs)]
    for copy in copies:
        copy.start()
    for copy in copies:
        copy.wait()


def on_device(Z, T, prompt, g1, wg1, wu1, wd1, g2, wg2, wu2, wd2):
    bf, f32 = jnp.bfloat16, jnp.float32
    X = T // CORES
    H = Z // 2
    rows, width = wg1.shape
    hid, dcol = wd1.shape
    tok, D = prompt.shape
    own = tok // Z
    rq = rows // X
    served = jax.ShapeDtypeStruct((Z, X, rq, hid), bf)
    down = jax.ShapeDtypeStruct((hid, D), bf)
    dma = pltpu.SemaphoreType.DMA
    ring = (2, 2, H, 2 * own, D // 2)
    anywhere = pl.BlockSpec(memory_space=pl.ANY)
    in_vmem = pl.BlockSpec(memory_space=pltpu.VMEM)
    held = pl.pallas_call(
        functools.partial(kernel, Z, T),
        out_shape=(pltpu.VMEM((4, Z, X, rq, hid), bf), pltpu.VMEM((2, hid, D), bf), pltpu.VMEM((tok, D), bf)),
        in_specs=[anywhere] * 9,
        out_specs=(in_vmem,) * 3,
        scratch_shapes=[
            pltpu.VMEM((tok, D), bf),
            pltpu.VMEM((2, 1, rows), f32),
            pltpu.VMEM((4, rows, width), f32),
            pltpu.VMEM((2, hid, dcol), f32),
            pltpu.VMEM((4, rows, width), bf),
            pltpu.VMEM((2, hid, dcol), bf),
            pltpu.VMEM((2, T, rq, width), bf),
            pltpu.VMEM((2, Z, rq, hid), bf),
            pltpu.VMEM((Z, 2 * own, D // 2), f32),
            pltpu.VMEM(ring[3:], f32),
            pltpu.VMEM(ring, bf), pltpu.VMEM(ring, bf),
            pltpu.VMEM((2, Z, 2 * own, D // 2), bf),
            dma((2,)), dma((2,)), dma((2,)), dma((2,)), dma((2,)), dma((2, X)), dma((2,)), dma((2,)), dma((2,)),
            dma((2, 2)), dma((2, 2, H)), dma((2, 2)), dma((2, 2, H)),
            dma((2,)), dma((9,)), pltpu.SemaphoreType.REGULAR((H.bit_length(),)),
        ],
        compiler_params=pltpu.CompilerParams(collective_id=0, has_side_effects=True, vmem_limit_bytes=VMEM - 2 * (4 * Z * X * rq * hid + 2 * hid * D + tok * D)),
        name="handoff",
    )(prompt, g1.reshape(1, rows), wg1, wu1, wd1, g2.reshape(1, rows), wg2, wu2, wd2)
    outs = pl.pallas_call(
        put_out,
        out_shape=(jax.ShapeDtypeStruct((tok, D), bf), served, served, down, served, served, down),
        in_specs=[in_vmem] * 3,
        out_specs=(anywhere,) * 7,
        scratch_shapes=[dma((7,))],
        compiler_params=pltpu.CompilerParams(vmem_limit_bytes=8 * 2**20),
        name="put_out",
    )(*held)
    flat = lambda a: a.reshape(-1, hid)
    return (outs[0], flat(outs[1]), flat(outs[2]), outs[3], flat(outs[4]), flat(outs[5]), outs[6])


def solution(mesh):
    return jax.shard_map(
        functools.partial(on_device, mesh.shape["fs"], mesh.shape["tp"]),
        mesh=mesh,
        in_specs=(
            P(("grp", "tp"), None),
            P("fs"),
            P("fs", "tp"),
            P("fs", "tp"),
            P("fs", "tp"),
            P("fs"),
            P("fs", "tp"),
            P("fs", "tp"),
            P("fs", "tp"),
        ),
        out_specs=(
            P(("grp", "tp"), None),
            P("grp", "fs"),
            P("grp", "fs"),
            P("fs", "grp"),
            P("grp", "fs"),
            P("grp", "fs"),
            P("fs", "grp"),
        ),
        check_vma=False,
    )
```
